32 devices in a mesh: sp: 8 (over z, y), dp: 4 (over x, core).
Axes of the slice: x: 2, y: 2, z: 4, core: 2. Of those that a mesh axis runs over, the one named last changes fastest.
Arguments:
- stream: bfloat16 [4, 1024, 2048], P('dp', 'sp'), may hold values from -6 to 6
- queries: bfloat16 [4, 1024, 1024], P('dp', 'sp'), may hold values from -6 to 6
- keys_in: bfloat16 [4, 1024, 1024], P('dp', 'sp'), may hold values from -6 to 6
- values_in: bfloat16 [4, 1024, 1024], P('dp', 'sp'), may hold values from -6 to 6
- key_shift: bfloat16 [4, 1024, 16], P('dp', 'sp'), may hold values from -8 to 16
- head_shift: float32 [16], replicated, may hold values from -16 to 0
- mix_gain: float32 [1024], replicated, may hold values from 0.1 to 1.9
- out_weight: bfloat16 [1024, 2048], replicated, may hold values from -0.1875 to 0.1875
- post_gain: float32 [2048], replicated, may hold values from 0.1 to 1.9
- route: int32 [4, 1024, 2], P('dp', 'sp'), may hold values from 0 to 31, as said below
- route_weight: float32 [4, 1024, 2], P('dp', 'sp'), may hold values from 0.25 to 1
- w_gate: bfloat16 [32, 2048, 1024], P(('sp', 'dp')), may hold values from -0.125 to 0.125
- w_up: bfloat16 [32, 2048, 1024], P(('sp', 'dp')), may hold values from -0.125 to 0.125
- w_down: bfloat16 [32, 1024, 2048], P(('sp', 'dp')), may hold values from -0.1875 to 0.1875
Outputs:
- result: bfloat16 [4, 1024, 2048], P('dp', 'sp')
The draws below stay inside these ranges and needn't reach their ends.
Inputs may be any that keep to these rules, and one draw needn't show every extreme that they name: `route`: each token names two different experts of one group (the group of expert e is e // 8). Of the 128 tokens of one device, each expert is named by at most 16; in every draw the 8 experts of one group are each named by exactly 16 tokens of every device.
All inputs are finite; a program needn't handle non-finite values.
Results may differ from the reference program's by a relative error of at most 0.0085.
Values may be sent and summed in bfloat16 or wider, within the bound.
A program may use at most 128 MiB of HBM per device.

```python
import math
import jax
import jax.numpy as jnp
from jax import lax

D = 2048
HEADS = 16
HD = 64
F = 1024
GROUPS = 4
TOK_DEV = 128
SEQUENCE_LENGTH = 1024
SEQUENCE_COUNT = 4
EXPERTS = 32
EPG = 8
CAP = 16
N_SP = 8
N_DP = 4


def head_rates(key):
    base = jax.random.fold_in(key, 11)
    share = jax.random.uniform(base, (HEADS,), jnp.float32, 0.4, 1.4)
    return -share * math.log(SEQUENCE_LENGTH)


def draw_head_shift(key, part):
    return head_rates(key)


def draw_key_shift(key, part):
    decay_rates = head_rates(key)
    random_jitter = jnp.clip(0.7 * jax.random.normal(jax.random.fold_in(key, 12), (SEQUENCE_COUNT, SEQUENCE_LENGTH // TOK_DEV, TOK_DEV, HEADS), jnp.float32), -3.0, 3.0)
    offset = jax.random.uniform(jax.random.fold_in(key, 13), (SEQUENCE_COUNT, SEQUENCE_LENGTH // TOK_DEV, 1, HEADS), jnp.float32, -0.7, 0.7)
    random_jitter = (random_jitter + offset).reshape(SEQUENCE_COUNT, SEQUENCE_LENGTH, HEADS)
    sudden_spike = jax.random.randint(jax.random.fold_in(key, 14), (SEQUENCE_COUNT, SEQUENCE_LENGTH, 1), 0, max(SEQUENCE_LENGTH // 4, 2)) == 0
    value_entry = jnp.where(sudden_spike, -decay_rates[None, None, :] - 0.7, random_jitter)
    return value_entry.astype(jnp.bfloat16)


def draw_route(key, part):
    nblocks = SEQUENCE_COUNT * (SEQUENCE_LENGTH // TOK_DEV)
    half = TOK_DEV // 2
    hot = jax.random.randint(jax.random.fold_in(key, 21), (), 0, GROUPS)
    cuts = jnp.sort(jax.random.randint(jax.random.fold_in(key, 22), (nblocks, GROUPS - 2), 0, half + 1), axis=1)
    bounds = jnp.concatenate([jnp.zeros((nblocks, 1), jnp.int32), cuts, jnp.full((nblocks, 1), half, jnp.int32)], axis=1)
    others = bounds[:, 1:] - bounds[:, :-1]
    sizes = jnp.concatenate([jnp.full((nblocks, 1), half, jnp.int32), others], axis=1)
    ends = jnp.cumsum(sizes, axis=1)
    starts = ends - sizes
    position = jnp.arange(TOK_DEV, dtype=jnp.int32)
    section = jnp.sum((position[None, :, None] >= ends[:, None, :]).astype(jnp.int32), axis=2)
    within = position[None, :] - jnp.take_along_axis(starts, section, axis=1)
    group = (hot + section) % GROUPS
    per_row = EPG // 2
    row_idx = within // per_row
    col_idx = within % per_row
    scores = jax.random.randint(jax.random.fold_in(key, 23), (nblocks, GROUPS, CAP, EPG), 0, 2 ** 20) * EPG + jnp.arange(EPG, dtype=jnp.int32)
    perm = jnp.argsort(scores, axis=-1, stable=True).astype(jnp.int32).reshape(nblocks, GROUPS * CAP * EPG)
    flat_idx = (section * CAP + row_idx) * EPG + 2 * col_idx
    first = jnp.take_along_axis(perm, flat_idx, axis=1) + group * EPG
    second = jnp.take_along_axis(perm, flat_idx + 1, axis=1) + group * EPG
    pairs = jnp.stack([first, second], axis=2)
    tscore = jax.random.randint(jax.random.fold_in(key, 24), (nblocks, TOK_DEV), 0, 2 ** 20) * TOK_DEV + position[None, :]
    placement = jnp.argsort(tscore, axis=1, stable=True).astype(jnp.int32)
    shuffled = jnp.take_along_axis(pairs, placement[:, :, None], axis=1)
    return shuffled.reshape(SEQUENCE_COUNT, SEQUENCE_LENGTH, 2).astype(jnp.int32)


def steps_of(rng, dims, cuts, low, high):
    loudness, own = 1.0, jax.random.fold_in(rng, 6)
    for axis_at, blocks in cuts:
        heights = jnp.exp(jax.random.uniform(jax.random.fold_in(own, axis_at), (blocks,), jnp.float32, low / len(cuts), high / len(cuts)))
        loudness = loudness * jnp.repeat(heights, dims[axis_at] // blocks).reshape([-1 if axis == axis_at else 1 for axis in range(len(dims))])
    return loudness


def noise(key, dims, scale, most, cuts=(), kind=jnp.bfloat16):
    drawn = scale * jax.random.normal(key, dims, jnp.float32)
    if cuts:
        drawn = drawn * steps_of(key, dims, cuts, -0.22, 0.18)
    return jnp.clip(drawn, -most, most).astype(kind)


def setup_inputs(seed: int = 0) -> dict:
    arg_keys = jax.random.split(jax.random.key(seed), 15)
    stream = noise(arg_keys[0], (SEQUENCE_COUNT, SEQUENCE_LENGTH, D), 1.0, 6.0, ((0, 4), (1, 8)))
    queries = noise(arg_keys[1], (SEQUENCE_COUNT, SEQUENCE_LENGTH, HEADS * HD), 1.0, 6.0, ((0, 4), (1, 8)))
    keys_in = noise(arg_keys[2], (SEQUENCE_COUNT, SEQUENCE_LENGTH, HEADS * HD), 1.0, 6.0, ((0, 4), (1, 8)))
    values_in = noise(arg_keys[3], (SEQUENCE_COUNT, SEQUENCE_LENGTH, HEADS * HD), 1.0, 6.0, ((0, 4), (1, 8)))
    key_shift = draw_key_shift(jax.random.fold_in(arg_keys[14], 71), 0)
    head_shift = draw_head_shift(jax.random.fold_in(arg_keys[14], 71), 0)
    mix_gain = jnp.clip(1.0 + 0.18 * jax.random.normal(arg_keys[6], (HEADS * HD,), jnp.float32), 0.1, 1.9)
    out_weight = noise(arg_keys[7], (HEADS * HD, D), (HEADS * HD) ** -0.5, 0.1875)
    post_gain = jnp.clip(1.0 + 0.18 * jax.random.normal(arg_keys[8], (D,), jnp.float32), 0.1, 1.9)
    route = draw_route(jax.random.fold_in(arg_keys[14], 71), 0)
    route_weight = jnp.clip(jnp.exp(math.log(1.0) - 1.3862944 * jax.random.uniform(arg_keys[10], (SEQUENCE_COUNT, SEQUENCE_LENGTH, 2), jnp.float32) ** steps_of(arg_keys[10], (SEQUENCE_COUNT, SEQUENCE_LENGTH, 2), ((0, 4), (1, 8)), -0.2, 0.2)), 0.25, 1.0)
    w_gate = noise(arg_keys[11], (EXPERTS, D, F), D ** -0.5, 0.125, ((0, 32),))
    w_up = noise(arg_keys[12], (EXPERTS, D, F), D ** -0.5, 0.125, ((0, 32),))
    w_down = noise(arg_keys[13], (EXPERTS, F, D), F ** -0.5, 0.1875, ((0, 32),))
    return dict(stream=stream, queries=queries, keys_in=keys_in, values_in=values_in, key_shift=key_shift, head_shift=head_shift, mix_gain=mix_gain, out_weight=out_weight, post_gain=post_gain, route=route, route_weight=route_weight, w_gate=w_gate, w_up=w_up, w_down=w_down)


norm_eps = 1e-05

def block_total(length):
    blocks = 1
    while blocks * 2 <= min(8, length // 512):
        blocks = blocks * 2
    return blocks

def stick_head(queries_head, keys_head, values_head, offsets):
    length = queries_head.shape[0]
    blocks = block_total(length)
    width = length // blocks
    scale = 1.0 / math.sqrt(HD)
    pieces = []
    for block_idx in range(blocks):
        begin = block_idx * width
        finish = begin + width
        logits = jnp.dot(queries_head[begin:finish].astype(jnp.float32), keys_head[:finish].astype(jnp.float32).T, precision=lax.Precision.HIGHEST, preferred_element_type=jnp.float32) * scale
        logits = logits + offsets[None, :finish]
        rows_pos = begin + jnp.arange(width, dtype=jnp.int32)
        cols_pos = jnp.arange(finish, dtype=jnp.int32)
        causal = cols_pos[None, :] < rows_pos[:, None]
        breaks = jnp.where(causal, jax.nn.log_sigmoid(-logits), 0.0)
        suffix = lax.cumsum(breaks, axis=1, reverse=True) - breaks
        weights = jnp.where(causal, jnp.exp(jax.nn.log_sigmoid(logits) + suffix), 0.0).astype(jnp.bfloat16)
        pieces.append(jnp.dot(weights.astype(jnp.float32), values_head[:finish].astype(jnp.float32), precision=lax.Precision.HIGHEST, preferred_element_type=jnp.float32))
    return jnp.concatenate(pieces, axis=0)

def reference(stream, queries, keys_in, values_in, key_shift, head_shift, mix_gain, out_weight, post_gain, route, route_weight, w_gate, w_up, w_down):

    def by_head(array):
        return array.reshape(SEQUENCE_COUNT, SEQUENCE_LENGTH, HEADS, HD).transpose(0, 2, 1, 3).reshape(SEQUENCE_COUNT * HEADS, SEQUENCE_LENGTH, HD)
    offsets = key_shift.astype(jnp.float32).transpose(0, 2, 1) + head_shift[None, :, None]
    offsets = offsets.reshape(SEQUENCE_COUNT * HEADS, SEQUENCE_LENGTH)

    def one_head(items):
        return stick_head(items[0], items[1], items[2], items[3]).astype(jnp.bfloat16)
    attended = lax.map(one_head, (by_head(queries), by_head(keys_in), by_head(values_in), offsets))
    attended = attended.reshape(SEQUENCE_COUNT, HEADS, SEQUENCE_LENGTH, HD).transpose(0, 2, 1, 3).reshape(SEQUENCE_COUNT * SEQUENCE_LENGTH, HEADS * HD)
    att32 = attended.astype(jnp.float32)
    normed = (att32 * lax.rsqrt(lax.optimization_barrier(jnp.mean(att32 * att32, axis=1, keepdims=True)) + norm_eps) * mix_gain).astype(jnp.bfloat16)
    mixed = jnp.dot(normed.astype(jnp.float32), out_weight.astype(jnp.float32), precision=lax.Precision.HIGHEST, preferred_element_type=jnp.float32)
    summed = stream.reshape(SEQUENCE_COUNT * SEQUENCE_LENGTH, D).astype(jnp.float32) + mixed
    hidden = (summed * lax.rsqrt(lax.optimization_barrier(jnp.mean(summed * summed, axis=1, keepdims=True)) + norm_eps) * post_gain).astype(jnp.bfloat16)
    total = SEQUENCE_COUNT * SEQUENCE_LENGTH
    expert_ids = route.reshape(total * 2).astype(jnp.int32)
    weights_flat = route_weight.reshape(total * 2)
    order = jnp.argsort(expert_ids, stable=True).astype(jnp.int32)
    tok_sorted = order // 2
    weight_sorted = weights_flat[order]
    counts = lax.optimization_barrier(jnp.sum((expert_ids[:, None] == jnp.arange(EXPERTS, dtype=jnp.int32)[None, :]).astype(jnp.int32), axis=0))
    starts = (jnp.cumsum(counts) - counts).astype(jnp.int32)
    most_rows = N_SP * N_DP * CAP
    tok_padded = jnp.concatenate([tok_sorted, jnp.zeros((most_rows,), jnp.int32)])
    weight_padded = jnp.concatenate([weight_sorted, jnp.zeros((most_rows,), jnp.float32)])

    def one_expert(carry, expert):
        index_rows = lax.dynamic_slice(tok_padded, (starts[expert],), (most_rows,))
        weight_rows = lax.dynamic_slice(weight_padded, (starts[expert],), (most_rows,))
        valid = jnp.arange(most_rows, dtype=jnp.int32) < counts[expert]
        rows = hidden[index_rows].astype(jnp.float32)
        gate = jnp.dot(rows, w_gate[expert].astype(jnp.float32), precision=lax.Precision.HIGHEST, preferred_element_type=jnp.float32)
        upper = jnp.dot(rows, w_up[expert].astype(jnp.float32), precision=lax.Precision.HIGHEST, preferred_element_type=jnp.float32)
        inner = (jax.nn.silu(gate) * upper).astype(jnp.bfloat16)
        output = jnp.dot(inner.astype(jnp.float32), w_down[expert].astype(jnp.float32), precision=lax.Precision.HIGHEST, preferred_element_type=jnp.float32).astype(jnp.bfloat16)
        scaled_values = jnp.where(valid[:, None], weight_rows[:, None] * output.astype(jnp.float32), 0.0)
        return (carry.at[index_rows].add(scaled_values), None)
    moe_sum, _ = lax.scan(one_expert, jnp.zeros((total, D), jnp.float32), jnp.arange(EXPERTS, dtype=jnp.int32))
    result = (hidden.astype(jnp.float32) + moe_sum).astype(jnp.bfloat16)
    return result.reshape(SEQUENCE_COUNT, SEQUENCE_LENGTH, D)
```

```python
import functools
import math

import jax
import jax.numpy as jnp
from jax import lax
from jax.experimental import pallas as pl
from jax.experimental.pallas import tpu as pltpu
from jax.sharding import PartitionSpec as P

HD = 64
GROUPS = 4
MESH = pl.DeviceIdType.MESH
F32 = jnp.float32
BF16 = jnp.bfloat16
VLIM = 56 * 1024 * 1024

norm_eps = 1e-05


def vmem(count):
    return [pl.BlockSpec(memory_space=pltpu.VMEM)] * count


def swap_kernel(n, count, *refs):
    ins, outs = refs[:count], refs[count : 2 * count]
    send_sem, recv_sem, own_sem = refs[2 * count :]
    me = lax.axis_index("sp")
    dp = lax.axis_index("dp")
    barrier = pltpu.get_barrier_semaphore()
    for d in range(1, n):
        pl.semaphore_signal(
            barrier, inc=1, device_id=(lax.rem(me + d, n), dp), device_id_type=MESH
        )
    own = [
        pltpu.make_async_copy(ins[a].at[me], outs[a].at[me], own_sem.at[a]) for a in range(count)
    ]
    for copy in own:
        copy.start()
    pl.semaphore_wait(barrier, n - 1)
    copies = []
    for d in range(1, n):
        peer = lax.rem(me + d, n)
        for a in range(count):
            copies.append(
                pltpu.make_async_remote_copy(
                    src_ref=ins[a].at[peer],
                    dst_ref=outs[a].at[me],
                    send_sem=send_sem.at[a, d],
                    recv_sem=recv_sem.at[a, d],
                    device_id=(peer, dp),
                    device_id_type=MESH,
                )
            )
            copies[-1].start()
    for copy in own + copies:
        copy.wait()


def swap(n, collective, *arrays):
    count = len(arrays)
    return pl.pallas_call(
        functools.partial(swap_kernel, n, count),
        out_shape=[jax.ShapeDtypeStruct(a.shape, a.dtype) for a in arrays],
        in_specs=vmem(count),
        out_specs=vmem(count),
        scratch_shapes=[
            pltpu.SemaphoreType.DMA((count, n)),
            pltpu.SemaphoreType.DMA((count, n)),
            pltpu.SemaphoreType.DMA((count,)),
        ],
        compiler_params=pltpu.CompilerParams(
            collective_id=collective, has_side_effects=True, vmem_limit_bytes=VLIM
        ),
        name=f"swap{collective}",
    )(*arrays)


def attention_kernel(heads, qkv_ref, shift_ref, out_ref):
    blocks, rows, _ = qkv_ref.shape
    cols = heads * HD
    scale = 1.0 / math.sqrt(HD)
    row = lax.broadcasted_iota(jnp.int32, (2 * rows, 2 * rows), 0)
    col = lax.broadcasted_iota(jnp.int32, (2 * rows, 2 * rows), 1)
    source = jnp.where(row >= rows, row - rows, row)
    summer = jnp.where((col >= rows) | (source > col), 1.0, 0.0).astype(BF16)
    causal = lax.broadcasted_iota(jnp.int32, (rows, rows), 1) < lax.broadcasted_iota(
        jnp.int32, (rows, rows), 0
    )

    def tile(i, j, h, carry, total, diagonal):
        q = qkv_ref[i, :, h * HD : (h + 1) * HD]
        k = qkv_ref[j, :, cols + h * HD : cols + (h + 1) * HD]
        v = qkv_ref[j, :, 2 * cols + h * HD : 2 * cols + (h + 1) * HD]
        z = lax.dot_general(q, k, (((1,), (1,)), ((), ())), preferred_element_type=F32) * scale
        z = z + shift_ref[j, h : h + 1, :]
        soft = jnp.log(1.0 + jnp.exp(-jnp.abs(z)))
        breaks = -jnp.maximum(z, 0.0) - soft
        own = jnp.minimum(z, 0.0) - soft
        if diagonal:
            breaks = jnp.where(causal, breaks, 0.0)
        high = breaks.astype(BF16)
        low = (breaks - high.astype(F32)).astype(BF16)
        sums = jnp.dot(
            jnp.concatenate([high, low], axis=1), summer, preferred_element_type=F32
        )
        weight = jnp.exp(own + (sums[:, :rows] + carry))
        if diagonal:
            weight = jnp.where(causal, weight, 0.0)
        total = total + jnp.dot(weight.astype(BF16), v, preferred_element_type=F32)
        return carry + sums[:, rows:], total

    zero_carry = jnp.zeros((rows, rows), F32)
    zero_total = jnp.zeros((rows, HD), F32)

    for i in range(blocks):
        state = []
        for h in range(heads):
            state.extend(tile(i, i, h, zero_carry, zero_total, True))
        for j in range(i - 1, -1, -1):
            new = []
            for h in range(heads):
                new.extend(tile(i, j, h, state[2 * h], state[2 * h + 1], False))
            state = new
        out_ref[i] = jnp.concatenate([state[2 * h + 1] for h in range(heads)], axis=1).astype(BF16)


def attention(heads, qkv, shift):
    blocks, rows, _ = qkv.shape
    return pl.pallas_call(
        functools.partial(attention_kernel, heads),
        out_shape=jax.ShapeDtypeStruct((blocks, rows, heads * HD), BF16),
        in_specs=vmem(2),
        out_specs=vmem(1)[0],
        compiler_params=pltpu.CompilerParams(vmem_limit_bytes=VLIM),
        name="attention",
    )(qkv, shift)


def place(n_sp, n_dp):
    ny = n_sp // GROUPS
    sp, dp = lax.axis_index("sp"), lax.axis_index("dp")
    plane, y = sp // ny, lax.rem(sp, ny)
    member = y * n_dp + dp

    def at(g, m):
        return (g * ny + m // n_dp, lax.rem(m, n_dp))

    return plane, member, at


def greet(plane, member, at, per_group):
    barrier = pltpu.get_barrier_semaphore()
    for d in range(1, GROUPS):
        pl.semaphore_signal(
            barrier, inc=1, device_id=at(lax.rem(plane + d, GROUPS), member), device_id_type=MESH
        )
    for d in range(1, per_group):
        pl.semaphore_signal(
            barrier, inc=1, device_id=at(plane, lax.rem(member + d, per_group)), device_id_type=MESH
        )
    pl.semaphore_wait(barrier, GROUPS + per_group - 2)


def one_hot_rows(meta, row):
    lanes = lax.broadcasted_iota(jnp.int32, (meta.shape[1], meta.shape[1]), 0).astype(F32)
    return lanes == meta[row : row + 1, :]


def moe_kernel(
    n_sp,
    n_dp,
    hidden,
    slot_hot,
    token_hot,
    meta,
    gate_hbm,
    up_hbm,
    down_hbm,
    result,
    packed,
    landed,
    tables,
    stage,
    got,
    inner,
    reply,
    back,
    partial,
    returned,
    gate_w,
    up_w,
    down_w,
    w_sem,
    t_send,
    t_recv,
    z_send,
    z_recv,
    p_send,
    p_recv,
    r_send,
    r_recv,
    y_send,
    y_recv,
):
    tokens, width = hidden.shape
    _, per_group, cap, _ = got.shape
    slots = packed.shape[1]
    lanes = per_group * cap
    ffn = inner.shape[1]
    chunk = min(512, width)
    chunks = [pl.ds(c, chunk) for c in range(0, width, chunk)]
    plane, member, at = place(n_sp, n_dp)

    loads = [
        pltpu.make_async_copy(gate_hbm, gate_w, w_sem.at[0]),
        pltpu.make_async_copy(up_hbm, up_w, w_sem.at[1]),
        pltpu.make_async_copy(down_hbm, down_w, w_sem.at[2]),
    ]
    for load in loads:
        load.start()
    greet(plane, member, at, per_group)

    flip = 1 - 2 * lax.rem(plane, 2)
    others = [plane, plane + flip, lax.rem(plane + 2, GROUPS), GROUPS - 1 - plane]

    def put_rows(ref, source, cols, rows):
        if cap % 16 == 0:
            ref[source, :, :, cols] = rows.astype(BF16).reshape(per_group, cap, chunk)
        else:
            for m in range(per_group):
                ref[source, m, :, cols] = rows[m * cap : (m + 1) * cap].astype(BF16)

    def take_rows(ref, source, cols):
        if cap % 16 == 0:
            rows = ref[source, :, :, cols]
            return rows.reshape(lanes, rows.shape[-1])
        return jnp.concatenate(
            [ref[source, m, :, cols].astype(F32) for m in range(per_group)], axis=0
        ).astype(BF16)

    sends = []

    def remote(src, dst, send, recv, device):
        copy = pltpu.make_async_remote_copy(
            src_ref=src,
            dst_ref=dst,
            send_sem=send,
            recv_sem=recv,
            device_id=device,
            device_id_type=MESH,
        )
        copy.start()
        return copy

    z_copies = {}
    for k in range(1, GROUPS):
        q = others[k]
        z_copies[k, -1] = remote(
            meta.at[q], tables.at[plane], t_send.at[k], t_recv.at[k], at(q, member)
        )
        hot = slot_hot[q]
        for c, cols in enumerate(chunks):
            packed[q, :, cols] = jnp.dot(
                hot, hidden[:, cols], preferred_element_type=F32
            ).astype(BF16)
            z_copies[k, c] = remote(
                packed.at[q, :, cols],
                landed.at[plane, :, cols],
                z_send.at[k, c],
                z_recv.at[k, c],
                at(q, member),
            )
    tables[plane] = meta[plane]
    hot = slot_hot[plane]
    for cols in chunks:
        landed[plane, :, cols] = jnp.dot(
            hot, hidden[:, cols], preferred_element_type=F32
        ).astype(BF16)

    def fan_out(source, src, dst, cols, send, recv):
        for e in range(1, per_group):
            other = lax.rem(member + e, per_group)
            remote(
                src.at[source, other, :, cols],
                dst.at[source, member, :, cols],
                send,
                recv,
                at(plane, other),
            )
        dst[source, member, :, cols] = src[source, member, :, cols]

    def group_wait(source, ref, cols, sem):
        part = ref.at[source, pl.ds(0, per_group - 1), :, cols]
        pltpu.make_async_copy(part, part, sem).wait()

    def deliver(k):
        source = others[k]
        if k:
            z_copies[k, -1].wait_recv()
        info = tables[source]
        hot = jnp.where(one_hot_rows(info, 0) | one_hot_rows(info, 1), 1.0, 0.0).astype(BF16)
        hot = hot[:, :slots]
        for c, cols in enumerate(chunks):
            if k:
                z_copies[k, c].wait_recv()
            rows = jnp.dot(hot, landed[source, :, cols], preferred_element_type=F32)
            put_rows(stage, source, cols, rows)
            fan_out(source, stage, got, cols, p_send.at[k, c], p_recv.at[k, c])

    def experts(k):
        source = others[k]
        for c, cols in enumerate(chunks):
            group_wait(source, got, cols, p_recv.at[k, c])
        if k == 0:
            for load in loads:
                load.wait()
        rows = take_rows(got, source, slice(None))
        part = min(256, ffn)
        for n in range(0, ffn, part):
            gate = jnp.dot(rows, gate_w[:, n : n + part], preferred_element_type=F32)
            upper = jnp.dot(rows, up_w[:, n : n + part], preferred_element_type=F32)
            inner[:, n : n + part] = (gate / (1.0 + jnp.exp(-gate)) * upper).astype(BF16)
        for c, cols in enumerate(chunks):
            out = jnp.dot(inner[...], down_w[:, cols], preferred_element_type=F32)
            put_rows(reply, source, cols, out)
            fan_out(source, reply, back, cols, r_send.at[k, c], r_recv.at[k, c])

    y_copies = {}

    def combine(k):
        source = others[k]
        info = tables[source]
        spread = jnp.where(one_hot_rows(info, 0), info[2:3, :], 0.0) + jnp.where(
            one_hot_rows(info, 1), info[3:4, :], 0.0
        )
        spread = spread.T[:slots]
        high = spread.astype(BF16)
        low = (spread - high.astype(F32)).astype(BF16)
        for c, cols in enumerate(chunks):
            group_wait(source, back, cols, r_recv.at[k, c])
            rows = take_rows(back, source, cols)
            total = jnp.dot(high, rows, preferred_element_type=F32) + jnp.dot(
                low, rows, preferred_element_type=F32
            )
            if k:
                partial[source, :, cols] = total.astype(BF16)
                y_copies[k, c] = remote(
                    partial.at[source, :, cols],
                    returned.at[plane, :, cols],
                    y_send.at[k, c],
                    y_recv.at[k, c],
                    at(source, member),
                )
            else:
                returned[source, :, cols] = total.astype(BF16)

    deliver(0)
    deliver(1)
    experts(0)
    deliver(2)
    experts(1)
    deliver(3)
    experts(2)
    combine(1)
    experts(3)
    combine(2)
    combine(0)
    combine(3)

    for c, cols in enumerate(chunks):
        for k in range(1, GROUPS):
            y_copies[k, c].wait_recv()
        rows = returned[:, :, cols].reshape(GROUPS * slots, chunk)
        total = jnp.dot(token_hot[...], rows, preferred_element_type=F32)
        result[:, cols] = (hidden[:, cols].astype(F32) + total).astype(BF16)

    for k in range(GROUPS):
        for c, cols in enumerate(chunks):
            if k:
                z_copies[k, c].wait_send()
                y_copies[k, c].wait_send()
            group_wait(others[k], stage, cols, p_send.at[k, c])
            group_wait(others[k], reply, cols, r_send.at[k, c])
        if k:
            z_copies[k, -1].wait_send()


def moe(n_sp, n_dp, cap, hidden, slot_hot, token_hot, meta, w_gate, w_up, w_down):
    per_group = n_sp * n_dp // GROUPS
    tokens, width = hidden.shape
    slots = slot_hot.shape[1]
    ffn = w_gate.shape[1]
    chunks = width // min(512, width)
    dma = pltpu.SemaphoreType.DMA
    wide = (GROUPS, per_group, cap, width)
    narrow = (GROUPS, slots, width)
    return pl.pallas_call(
        functools.partial(moe_kernel, n_sp, n_dp),
        out_shape=jax.ShapeDtypeStruct((tokens, width), BF16),
        in_specs=vmem(4) + [pl.BlockSpec(memory_space=pl.ANY)] * 3,
        out_specs=vmem(1)[0],
        scratch_shapes=[
            pltpu.VMEM(narrow, BF16),
            pltpu.VMEM(narrow, BF16),
            pltpu.VMEM(meta.shape, F32),
            pltpu.VMEM(wide, BF16),
            pltpu.VMEM(wide, BF16),
            pltpu.VMEM((per_group * cap, ffn), BF16),
            pltpu.VMEM(wide, BF16),
            pltpu.VMEM(wide, BF16),
            pltpu.VMEM(narrow, BF16),
            pltpu.VMEM(narrow, BF16),
            pltpu.VMEM(w_gate.shape, BF16),
            pltpu.VMEM(w_up.shape, BF16),
            pltpu.VMEM(w_down.shape, BF16),
            dma((3,)),
            dma((GROUPS,)),
            dma((GROUPS,)),
            dma((GROUPS, chunks)),
            dma((GROUPS, chunks)),
            dma((GROUPS, chunks)),
            dma((GROUPS, chunks)),
            dma((GROUPS, chunks)),
            dma((GROUPS, chunks)),
            dma((GROUPS, chunks)),
            dma((GROUPS, chunks)),
        ],
        compiler_params=pltpu.CompilerParams(
            collective_id=2, has_side_effects=True, vmem_limit_bytes=VLIM
        ),
        name="moe",
    )(hidden, slot_hot, token_hot, meta, w_gate, w_up, w_down)


def on_device(
    n_sp,
    n_dp,
    stream,
    queries,
    keys_in,
    values_in,
    key_shift,
    head_shift,
    mix_gain,
    out_weight,
    post_gain,
    route,
    route_weight,
    w_gate,
    w_up,
    w_down,
):
    tokens, width = stream.shape[1], stream.shape[2]
    heads = key_shift.shape[2] // n_sp
    cols = heads * HD

    n_expert = n_sp * n_dp
    per_group = n_expert // GROUPS
    cap = tokens // per_group
    slots = tokens // 2
    expert_ids = route[0].reshape(tokens * 2)
    onehot = (expert_ids[:, None] == jnp.arange(n_expert, dtype=jnp.int32)[None, :]).astype(BF16)
    before = jnp.arange(tokens * 2)
    earlier = (before[:, None] > before[None, :]).astype(BF16)
    counts = jnp.dot(earlier, onehot, preferred_element_type=F32)
    ranks = jnp.sum(counts * onehot.astype(F32), axis=1)
    inside = lax.rem(expert_ids, per_group).astype(F32) * cap + ranks
    inside = inside.reshape(tokens, 2)
    token_group = route[0][:, 0] // per_group
    group_hot = (token_group[:, None] == jnp.arange(GROUPS, dtype=jnp.int32)[None, :]).astype(BF16)
    group_rank = jnp.sum(
        jnp.dot(earlier[:tokens, :tokens], group_hot, preferred_element_type=F32)
        * group_hot.astype(F32),
        axis=1,
    )
    slot = token_group * slots + group_rank.astype(jnp.int32)
    slot_hot = slot[None, :] == jnp.arange(GROUPS * slots, dtype=jnp.int32)[:, None]
    facts = jnp.concatenate([inside + 1.0, route_weight[0]], axis=1)
    table = jnp.sum(jnp.where(slot_hot[:, None, :], facts.T[None, :, :], 0.0), axis=2)
    table = table - jnp.array([1.0, 1.0, 0.0, 0.0], F32)[None, :]
    table = table.reshape(GROUPS, slots, 4).transpose(0, 2, 1)
    lanes = per_group * cap
    meta = jnp.full((GROUPS, 8, lanes), -1.0, F32).at[:, :4, :slots].set(table)

    def by_peer(array):
        return array[0].reshape(tokens, n_sp, cols).transpose(1, 0, 2)

    qkv = jnp.concatenate([by_peer(queries), by_peer(keys_in), by_peer(values_in)], axis=2)
    offsets = (key_shift[0].astype(F32) + head_shift[None, :]).T.reshape(n_sp, heads, tokens)
    offsets = jnp.pad(offsets, ((0, 0), (0, 8 - heads), (0, 0)))
    qkv, offsets = swap(n_sp, 0, qkv, offsets)
    attended = attention(heads, qkv, offsets)
    (attended,) = swap(n_sp, 1, attended)
    att32 = attended.transpose(1, 0, 2).reshape(tokens, n_sp * cols).astype(F32)
    normed = (
        att32 * lax.rsqrt(jnp.mean(att32 * att32, axis=1, keepdims=True) + norm_eps) * mix_gain
    ).astype(BF16)
    mixed = jnp.dot(normed, out_weight, preferred_element_type=F32)
    summed = stream[0].astype(F32) + mixed
    hidden = (
        summed * lax.rsqrt(jnp.mean(summed * summed, axis=1, keepdims=True) + norm_eps) * post_gain
    ).astype(BF16)

    slot_hot = slot_hot.astype(BF16)
    out = moe(
        n_sp,
        n_dp,
        cap,
        hidden,
        slot_hot.reshape(GROUPS, slots, tokens),
        slot_hot.T,
        meta,
        w_gate[0],
        w_up[0],
        w_down[0],
    )
    return out[None]


def solution(mesh):
    return jax.shard_map(
        functools.partial(on_device, mesh.shape["sp"], mesh.shape["dp"]),
        mesh=mesh,
        in_specs=(
            P("dp", "sp", None),
            P("dp", "sp", None),
            P("dp", "sp", None),
            P("dp", "sp", None),
            P("dp", "sp", None),
            P(),
            P(),
            P(),
            P(),
            P("dp", "sp", None),
            P("dp", "sp", None),
            P(("sp", "dp"), None, None),
            P(("sp", "dp"), None, None),
            P(("sp", "dp"), None, None),
        ),
        out_specs=P("dp", "sp", None),
        check_vma=False,
    )
```

```python
import functools
import math

import jax
import jax.numpy as jnp
from jax import lax
from jax.experimental import pallas as pl
from jax.experimental.pallas import tpu as pltpu
from jax.sharding import PartitionSpec as P

HD = 64
GROUPS = 4
MESH = pl.DeviceIdType.MESH
F32 = jnp.float32
BF16 = jnp.bfloat16
VLIM = 60 * 1024 * 1024
LOG2E = math.log2(math.e)

norm_eps = 1e-05


def one_hot_rows(meta, row):
    lanes = lax.broadcasted_iota(jnp.int32, (meta.shape[1], meta.shape[1]), 0).astype(F32)
    return lanes == meta[row : row + 1, :]


def ones_where(mask):
    return jnp.where(mask, 1.0, 0.0).astype(BF16)


def layer_kernel(
    n_sp,
    n_dp,
    queries,
    keys_in,
    values_in,
    key_shift,
    head_shift,
    mix_gain,
    out_hbm,
    post_gain,
    stream_hbm,
    route,
    route_weight,
    gate_hbm,
    up_hbm,
    down_hbm,
    result,
    q_own,
    k_own,
    v_own,
    outbox,
    inbox,
    shift_pad,
    shift_out,
    shift_in,
    q_all,
    k_all,
    v_all,
    att_out,
    att_in,
    att,
    stream,
    summed,
    hidden,
    meta,
    slot_hot,
    token_hot,
    packed,
    landed,
    tables,
    stage,
    got,
    inner,
    reply,
    back,
    partial,
    returned,
    out_w,
    gate_w,
    up_w,
    down_w,
    i_sem,
    w_sem,
    s_send,
    s_recv,
    q_send,
    q_recv,
    a_send,
    a_recv,
    t_send,
    t_recv,
    z_send,
    z_recv,
    p_send,
    p_recv,
    r_send,
    r_recv,
    y_send,
    y_recv,
):
    tokens, width = hidden.shape
    heads = inbox.shape[0]
    half = tokens // 2
    _, per_group, cap, _ = got.shape
    slots = packed.shape[1]
    lanes = per_group * cap
    ffn = inner.shape[1]
    chunk = min(512, width)
    chunks = [pl.ds(c, chunk) for c in range(0, width, chunk)]
    me, dp = lax.axis_index("sp"), lax.axis_index("dp")
    ny = n_sp // GROUPS
    plane, y = me // ny, lax.rem(me, ny)
    member = y * n_dp + dp
    flip = 1 - 2 * lax.rem(plane, 2)
    others = [plane, plane + flip, lax.rem(plane + 2, GROUPS), GROUPS - 1 - plane]

    def at(g, m):
        return (g * ny + m // n_dp, lax.rem(m, n_dp))

    def remote(src, dst, send, recv, device):
        copy = pltpu.make_async_remote_copy(
            src_ref=src,
            dst_ref=dst,
            send_sem=send,
            recv_sem=recv,
            device_id=device,
            device_id_type=MESH,
        )
        copy.start()
        return copy

    def settle(part, sem):
        pltpu.make_async_copy(part, part, sem).wait()

    qkv_loads = [
        pltpu.make_async_copy(queries, q_own, i_sem.at[0]),
        pltpu.make_async_copy(keys_in, k_own, i_sem.at[1]),
        pltpu.make_async_copy(values_in, v_own, i_sem.at[2]),
    ]
    for load in qkv_loads:
        load.start()
    barrier = pltpu.get_barrier_semaphore()
    for d in range(1, n_sp):
        pl.semaphore_signal(
            barrier, inc=1, device_id=(lax.rem(me + d, n_sp), dp), device_id_type=MESH
        )
    for d in range(1, n_dp):
        for row in range(ny):
            pl.semaphore_signal(
                barrier,
                inc=1,
                device_id=(plane * ny + row, lax.rem(dp + d, n_dp)),
                device_id_type=MESH,
            )

    n_heads = key_shift.shape[1]
    shift_pad[...] = jnp.zeros_like(shift_pad)
    shift_pad[:, :n_heads] = (key_shift[...].astype(F32) + head_shift[...]) * LOG2E
    turned = shift_pad[...].T
    for p in range(n_sp):
        shift_out[p, :heads, :] = turned[p * heads : (p + 1) * heads]
    shift_in[me] = shift_out[me]

    for load in qkv_loads:
        load.wait()
    weight_loads = [
        pltpu.make_async_copy(stream_hbm, stream, w_sem.at[0]),
        pltpu.make_async_copy(out_hbm, out_w, w_sem.at[1]),
        pltpu.make_async_copy(gate_hbm, gate_w, w_sem.at[2]),
        pltpu.make_async_copy(up_hbm, up_w, w_sem.at[3]),
        pltpu.make_async_copy(down_hbm, down_w, w_sem.at[4]),
    ]
    for load in weight_loads:
        load.start()

    def pack_head(h):
        for p in range(n_sp):
            g = p * heads + h
            cols = slice(g * HD, (g + 1) * HD)
            outbox[h, p, :tokens, :] = jnp.concatenate([q_own[:, cols], k_own[:, cols]], axis=1)
            outbox[h, p, tokens:, :] = jnp.concatenate(
                [v_own[:half, cols], v_own[half:, cols]], axis=1
            )
        inbox[h, me] = outbox[h, me]

    order = sorted(range(1, n_sp), key=lambda d: abs(2 * d - n_sp))

    def send_head(h):
        for d in order:
            peer = lax.rem(me + d, n_sp)
            remote(
                outbox.at[h, peer], inbox.at[h, me], q_send.at[h], q_recv.at[h], (peer, dp)
            )

    pack_head(0)
    pl.semaphore_wait(barrier, n_sp - 1 + (n_dp - 1) * ny)
    for d in order:
        peer = lax.rem(me + d, n_sp)
        remote(shift_out.at[peer], shift_in.at[me], s_send.at[0], s_recv.at[0], (peer, dp))
    send_head(0)
    for h in range(1, heads):
        pack_head(h)
        send_head(h)

    row = lax.broadcasted_iota(jnp.int32, (tokens, tokens), 0)
    col = lax.broadcasted_iota(jnp.int32, (tokens, tokens), 1)
    earlier = ones_where(row > col)
    n_expert = n_sp * n_dp
    wide = max(tokens, n_expert)
    expert = lax.broadcasted_iota(jnp.int32, (tokens, wide), 1)
    first, second = route[:, 0:1], route[:, 1:2]
    hit0, hit1 = first == expert, second == expert
    count0 = jnp.dot(earlier, ones_where(hit0), preferred_element_type=F32)
    count1 = jnp.dot(earlier, ones_where(hit1), preferred_element_type=F32) + jnp.dot(
        jnp.ones((tokens, tokens), BF16), ones_where(hit0), preferred_element_type=F32
    )
    rank0 = jnp.sum(jnp.where(hit0, count0, 0.0), axis=1, keepdims=True)
    rank1 = jnp.sum(jnp.where(hit1, count1, 0.0), axis=1, keepdims=True)
    group = jnp.zeros((tokens, 1), F32)
    for g in range(1, GROUPS):
        group = group + jnp.where(first >= g * per_group, 1.0, 0.0)
    lane = col.astype(F32)
    in_group = lane == group
    group_count = jnp.dot(earlier, ones_where(in_group), preferred_element_type=F32)
    group_rank = jnp.sum(jnp.where(in_group, group_count, 0.0), axis=1, keepdims=True)
    base = group * per_group
    facts = [
        (first.astype(F32) - base) * cap + rank0 + 1.0,
        (second.astype(F32) - base) * cap + rank1 + 1.0,
        route_weight[:, 0:1],
        route_weight[:, 1:2],
    ]
    slot = group * slots + group_rank
    by_lane = jnp.broadcast_to(slot, (tokens, tokens)).T
    slot_row = lax.broadcasted_iota(jnp.int32, (slots, tokens), 0).astype(F32)
    token_hot[...] = ones_where(
        slot == lax.broadcasted_iota(jnp.int32, (tokens, GROUPS * slots), 1).astype(F32)
    )
    for g in range(GROUPS):
        slot_hot[g] = ones_where(by_lane[:slots] - float(g * slots) == slot_row)
        hot = (slot - float(g * slots) == lane) & (col < slots)
        rows = [jnp.sum(jnp.where(hot, f, 0.0), axis=0, keepdims=True) for f in facts]
        rows = [rows[0] - 1.0, rows[1] - 1.0, rows[2], rows[3]]
        meta[g] = jnp.concatenate(rows + [jnp.zeros((4, tokens), F32)], axis=0)
    tables[plane] = meta[plane]

    wide_source = lax.broadcasted_iota(jnp.int32, (2 * tokens, 2 * tokens), 0)
    wide_col = lax.broadcasted_iota(jnp.int32, (2 * tokens, 2 * tokens), 1)
    source = jnp.where(wide_source >= tokens, wide_source - tokens, wide_source)
    summer = jnp.where((wide_col >= tokens) | (source > wide_col), -1.0, 0.0).astype(BF16)
    pair = 2 if n_sp % 2 == 0 else 1
    span = pair * tokens
    tile_row = lax.broadcasted_iota(jnp.int32, (span, tokens), 0)
    tile_col = lax.broadcasted_iota(jnp.int32, (span, tokens), 1)
    scale = LOG2E / math.sqrt(HD)

    def attend(h, i):
        q = q_all[h, i * span : (i + 1) * span]
        carry = jnp.zeros((span, tokens), F32)
        total = jnp.zeros((span, HD), F32)
        for j in range(i, -1, -1):
            k = k_all[h, j * span : (j + 1) * span]
            z_pair = lax.dot_general(q, k, (((1,), (1,)), ((), ())), preferred_element_type=F32)
            parts = [None] * pair
            for b in range(pair - 1, -1, -1):
                z = z_pair[:, b * tokens : (b + 1) * tokens] * scale
                z = z + shift_in[j * pair + b, h : h + 1, :]
                soft = jnp.maximum(z, 0.0) + jnp.log2(1.0 + jnp.exp2(-jnp.abs(z)))
                own = z - soft
                if i == j:
                    causal = tile_col + b * tokens < tile_row
                    soft = jnp.where(causal, soft, 0.0)
                high = soft.astype(BF16)
                low = (soft - high.astype(F32)).astype(BF16)
                sums = jnp.dot(
                    jnp.concatenate([high, low], axis=1), summer, preferred_element_type=F32
                )
                weight = jnp.exp2(own + (sums[:, :tokens] + carry))
                if i == j:
                    weight = jnp.where(causal, weight, 0.0)
                carry = carry + sums[:, tokens:]
                parts[b] = weight.astype(BF16)
            total = total + jnp.dot(
                jnp.concatenate(parts, axis=1) if pair > 1 else parts[0],
                v_all[h, j * span : (j + 1) * span],
                preferred_element_type=F32,
            )
        for b in range(pair):
            t = i * pair + b
            block = total[b * tokens : (b + 1) * tokens]
            att_out[h, t] = jnp.concatenate([block[:half], block[half:]], axis=1).astype(BF16)
        for b in range(pair):
            t = i * pair + b

            @pl.when(me != t)
            def _(t=t):
                remote(
                    att_out.at[h, t], att_in.at[h, me], a_send.at[h], a_recv.at[h], (t, dp)
                )

            @pl.when(me == t)
            def _(t=t):
                att_in[h, t] = att_out[h, t]

    settle(shift_in.at[pl.ds(0, n_sp - 1)], s_recv.at[0])
    for h in range(heads):
        settle(inbox.at[h, pl.ds(0, n_sp - 1)], q_recv.at[h])
        for j in range(n_sp):
            here = slice(j * tokens, (j + 1) * tokens)
            q_all[h, here] = inbox[h, j, :tokens, :HD]
            k_all[h, here] = inbox[h, j, :tokens, HD:]
            v_all[h, j * tokens : j * tokens + half] = inbox[h, j, tokens:, :HD]
            v_all[h, j * tokens + half : (j + 1) * tokens] = inbox[h, j, tokens:, HD:]
        for i in range(n_sp // pair - 1, -1, -1):
            attend(h, i)

    for h in range(heads):
        settle(att_in.at[h, pl.ds(0, n_sp - 1)], a_recv.at[h])
        for p in range(n_sp):
            g = p * heads + h
            block = att_in[h, p]
            att[:half, g * HD : (g + 1) * HD] = block[:, :HD]
            att[half:, g * HD : (g + 1) * HD] = block[:, HD:]
    wide_att = att[...].astype(F32)
    ratio = lax.rsqrt(jnp.mean(wide_att * wide_att, axis=1, keepdims=True) + norm_eps)
    normed = (wide_att * ratio * mix_gain[...]).astype(BF16)
    weight_loads[0].wait()
    weight_loads[1].wait()
    square = jnp.zeros((tokens, 1), F32)
    for cols in chunks:
        block = stream[:, cols].astype(F32) + jnp.dot(
            normed, out_w[:, cols], preferred_element_type=F32
        )
        summed[:, cols] = block
        square = square + jnp.sum(block * block, axis=1, keepdims=True)
    ratio = lax.rsqrt(square / width + norm_eps)
    for cols in chunks:
        hidden[:, cols] = (summed[:, cols] * ratio * post_gain[:, cols]).astype(BF16)

    def put_rows(ref, source, cols, rows):
        if cap % 16 == 0:
            ref[source, :, :, cols] = rows.astype(BF16).reshape(per_group, cap, chunk)
        else:
            for m in range(per_group):
                ref[source, m, :, cols] = rows[m * cap : (m + 1) * cap].astype(BF16)

    def take_rows(ref, source, cols):
        if cap % 16 == 0:
            rows = ref[source, :, :, cols]
            return rows.reshape(lanes, rows.shape[-1])
        return jnp.concatenate(
            [ref[source, m, :, cols].astype(F32) for m in range(per_group)], axis=0
        ).astype(BF16)

    z_copies = {}

    def send_plane(k, c):
        q = others[k]
        packed[q, :, chunks[c]] = jnp.dot(
            slot_hot[q], hidden[:, chunks[c]], preferred_element_type=F32
        ).astype(BF16)
        z_copies[k, c] = remote(
            packed.at[q, :, chunks[c]],
            landed.at[plane, :, chunks[c]],
            z_send.at[k, c],
            z_recv.at[k, c],
            at(q, member),
        )

    pieces = range(len(chunks))
    for k in range(1, GROUPS):
        z_copies[k, -1] = remote(
            meta.at[others[k]],
            tables.at[plane],
            t_send.at[k],
            t_recv.at[k],
            at(others[k], member),
        )
    for c in pieces:
        send_plane(3, c)
        send_plane(1, c)
    for c in pieces:
        send_plane(2, c)
    for cols in chunks:
        landed[plane, :, cols] = jnp.dot(
            slot_hot[plane], hidden[:, cols], preferred_element_type=F32
        ).astype(BF16)

    def fan_out(source, src, dst, cols, send, recv):
        for e in range(1, per_group):
            other = lax.rem(member + e, per_group)
            remote(
                src.at[source, other, :, cols],
                dst.at[source, member, :, cols],
                send,
                recv,
                at(plane, other),
            )
        dst[source, member, :, cols] = src[source, member, :, cols]

    def group_wait(source, ref, cols, sem):
        settle(ref.at[source, pl.ds(0, per_group - 1), :, cols], sem)

    hots = {}

    def deliver(k, c):
        source = others[k]
        if k not in hots:
            if k:
                z_copies[k, -1].wait_recv()
            info = tables[source]
            hots[k] = ones_where(one_hot_rows(info, 0) | one_hot_rows(info, 1))[:, :slots]
        if k:
            z_copies[k, c].wait_recv()
        rows = jnp.dot(hots[k], landed[source, :, chunks[c]], preferred_element_type=F32)
        put_rows(stage, source, chunks[c], rows)
        fan_out(source, stage, got, chunks[c], p_send.at[k, c], p_recv.at[k, c])

    loaded = []

    def experts(k, send):
        source = others[k]
        for c, cols in enumerate(chunks):
            group_wait(source, got, cols, p_recv.at[k, c])
        if not loaded:
            loaded.append(True)
            for load in weight_loads[2:]:
                load.wait()
        rows = take_rows(got, source, slice(None))
        part = min(256, ffn)
        for n in range(0, ffn, part):
            gate = jnp.dot(rows, gate_w[:, n : n + part], preferred_element_type=F32)
            upper = jnp.dot(rows, up_w[:, n : n + part], preferred_element_type=F32)
            inner[:, n : n + part] = (gate / (1.0 + jnp.exp(-gate)) * upper).astype(BF16)
        for c, cols in enumerate(chunks):
            out = jnp.dot(inner[...], down_w[:, cols], preferred_element_type=F32)
            put_rows(reply, source, cols, out)
            if send:
                answer(k, c)

    def answer(k, c):
        fan_out(others[k], reply, back, chunks[c], r_send.at[k, c], r_recv.at[k, c])

    y_copies = {}

    def combine(k):
        source = others[k]
        info = tables[source]
        spread = jnp.where(one_hot_rows(info, 0), info[2:3, :], 0.0) + jnp.where(
            one_hot_rows(info, 1), info[3:4, :], 0.0
        )
        spread = spread.T[:slots]
        high = spread.astype(BF16)
        low = (spread - high.astype(F32)).astype(BF16)
        for c, cols in enumerate(chunks):
            group_wait(source, back, cols, r_recv.at[k, c])
            rows = take_rows(back, source, cols)
            total = jnp.dot(high, rows, preferred_element_type=F32) + jnp.dot(
                low, rows, preferred_element_type=F32
            )
            if k:
                partial[source, :, cols] = total.astype(BF16)
                y_copies[k, c] = remote(
                    partial.at[source, :, cols],
                    returned.at[plane, :, cols],
                    y_send.at[k, c],
                    y_recv.at[k, c],
                    at(source, member),
                )
            else:
                returned[source, :, cols] = total.astype(BF16)

    for c in pieces:
        deliver(0, c)
    for c in pieces:
        deliver(1, c)
        deliver(3, c)
    experts(0, False)
    experts(3, True)
    split = len(chunks) // 2
    for c in pieces[:split]:
        deliver(2, c)
    experts(1, True)
    for c in pieces[split:]:
        deliver(2, c)
    combine(3)
    experts(2, True)
    for c in pieces:
        answer(0, c)
    combine(1)
    combine(2)
    combine(0)

    for c, cols in enumerate(chunks):
        for k in range(1, GROUPS):
            y_copies[k, c].wait_recv()
        rows = returned[:, :, cols].reshape(GROUPS * slots, chunk)
        total = jnp.dot(token_hot[...], rows, preferred_element_type=F32)
        result[:, cols] = (hidden[:, cols].astype(F32) + total).astype(BF16)

    settle(shift_out.at[pl.ds(0, n_sp - 1)], s_send.at[0])
    for h in range(heads):
        settle(outbox.at[h, pl.ds(0, n_sp - 1)], q_send.at[h])
        settle(att_out.at[h, pl.ds(0, n_sp - 1)], a_send.at[h])
    for k in range(GROUPS):
        for c, cols in enumerate(chunks):
            if k:
                z_copies[k, c].wait_send()
                y_copies[k, c].wait_send()
            group_wait(others[k], stage, cols, p_send.at[k, c])
            group_wait(others[k], reply, cols, r_send.at[k, c])
        if k:
            z_copies[k, -1].wait_send()


def on_device(
    n_sp,
    n_dp,
    stream,
    queries,
    keys_in,
    values_in,
    key_shift,
    head_shift,
    mix_gain,
    out_weight,
    post_gain,
    route,
    route_weight,
    w_gate,
    w_up,
    w_down,
):
    tokens, width = stream.shape[1:]
    n_heads = key_shift.shape[2]
    heads = n_heads // n_sp
    mixer = queries.shape[2]
    ffn = w_gate.shape[2]
    per_group = n_sp * n_dp // GROUPS
    cap = tokens // per_group
    slots = tokens // 2
    chunks = width // min(512, width)
    dma = pltpu.SemaphoreType.DMA
    own = pltpu.VMEM((tokens, mixer), BF16)
    box = pltpu.VMEM((heads, n_sp, tokens + tokens // 2, 2 * HD), BF16)
    shifts = pltpu.VMEM((n_sp, 8, tokens), F32)
    line = pltpu.VMEM((heads, n_sp * tokens, HD), BF16)
    att_box = pltpu.VMEM((heads, n_sp, tokens // 2, 2 * HD), BF16)
    table = pltpu.VMEM((GROUPS, 8, tokens), F32)
    wide = pltpu.VMEM((GROUPS, per_group, cap, width), BF16)
    narrow = pltpu.VMEM((GROUPS, slots, width), BF16)
    here = pl.BlockSpec(memory_space=pltpu.VMEM)
    there = pl.BlockSpec(memory_space=pl.ANY)
    out = pl.pallas_call(
        functools.partial(layer_kernel, n_sp, n_dp),
        out_shape=jax.ShapeDtypeStruct((tokens, width), BF16),
        in_specs=[there] * 3 + [here] * 3 + [there, here, there, here, here] + [there] * 3,
        out_specs=here,
        scratch_shapes=[
            own,
            own,
            own,
            box,
            box,
            pltpu.VMEM((tokens, tokens), F32),
            shifts,
            shifts,
            line,
            line,
            line,
            att_box,
            att_box,
            own,
            pltpu.VMEM((tokens, width), BF16),
            pltpu.VMEM((tokens, width), F32),
            pltpu.VMEM((tokens, width), BF16),
            table,
            pltpu.VMEM((GROUPS, slots, tokens), BF16),
            pltpu.VMEM((tokens, GROUPS * slots), BF16),
            narrow,
            narrow,
            table,
            wide,
            wide,
            pltpu.VMEM((per_group * cap, ffn), BF16),
            wide,
            wide,
            narrow,
            narrow,
            pltpu.VMEM((mixer, width), BF16),
            pltpu.VMEM((width, ffn), BF16),
            pltpu.VMEM((width, ffn), BF16),
            pltpu.VMEM((ffn, width), BF16),
            dma((3,)),
            dma((5,)),
            dma((1,)),
            dma((1,)),
            dma((heads,)),
            dma((heads,)),
            dma((heads,)),
            dma((heads,)),
            dma((GROUPS,)),
            dma((GROUPS,)),
        ]
        + [dma((GROUPS, chunks))] * 8,
        compiler_params=pltpu.CompilerParams(
            collective_id=0, has_side_effects=True, vmem_limit_bytes=VLIM
        ),
        name="layer",
    )(
        queries[0],
        keys_in[0],
        values_in[0],
        key_shift[0],
        head_shift[None],
        mix_gain[None],
        out_weight,
        post_gain[None],
        stream[0],
        route[0],
        route_weight[0],
        w_gate[0],
        w_up[0],
        w_down[0],
    )
    return out[None]


def solution(mesh):
    return jax.shard_map(
        functools.partial(on_device, mesh.shape["sp"], mesh.shape["dp"]),
        mesh=mesh,
        in_specs=(
            P("dp", "sp", None),
            P("dp", "sp", None),
            P("dp", "sp", None),
            P("dp", "sp", None),
            P("dp", "sp", None),
            P(),
            P(),
            P(),
            P(),
            P("dp", "sp", None),
            P("dp", "sp", None),
            P(("sp", "dp"), None, None),
            P(("sp", "dp"), None, None),
            P(("sp", "dp"), None, None),
        ),
        out_specs=P("dp", "sp", None),
        check_vma=False,
    )
```

```python
import functools
import math

import jax
import jax.numpy as jnp
from jax import lax
from jax.experimental import pallas as pl
from jax.experimental.pallas import tpu as pltpu
from jax.sharding import PartitionSpec as P

HD = 64
GROUPS = 4
MESH = pl.DeviceIdType.MESH
F32 = jnp.float32
BF16 = jnp.bfloat16
VLIM = 60 * 1024 * 1024
LOG2E = math.log2(math.e)

norm_eps = 1e-05


def one_hot_rows(meta, row):
    lanes = lax.broadcasted_iota(jnp.int32, (meta.shape[1], meta.shape[1]), 0).astype(F32)
    return lanes == meta[row : row + 1, :]


def ones_where(mask):
    return jnp.where(mask, 1.0, 0.0).astype(BF16)


def layer_kernel(
    n_sp,
    n_dp,
    queries,
    keys_in,
    values_in,
    key_shift_hbm,
    head_shift_hbm,
    mix_gain_hbm,
    out_hbm,
    post_gain_hbm,
    stream_hbm,
    route_hbm,
    route_weight_hbm,
    gate_hbm,
    up_hbm,
    down_hbm,
    result,
    key_shift,
    head_shift,
    mix_gain,
    post_gain,
    route,
    route_weight,
    q_own,
    k_own,
    v_own,
    outbox,
    inbox,
    shift_out,
    shift_in,
    q_all,
    k_all,
    v_all,
    att_out,
    att_in,
    att,
    stream,
    summed,
    hidden,
    meta,
    slot_hot,
    token_hot,
    packed,
    landed,
    tables,
    stage,
    got,
    inner,
    reply,
    back,
    partial,
    returned,
    out_w,
    gate_w,
    up_w,
    down_w,
    i_sem,
    n_sem,
    w_sem,
    s_send,
    s_recv,
    q_send,
    q_recv,
    a_send,
    a_recv,
    t_send,
    t_recv,
    z_send,
    z_recv,
    p_send,
    p_recv,
    r_send,
    r_recv,
    y_send,
    y_recv,
):
    tokens, width = hidden.shape
    heads = inbox.shape[0]
    half = tokens // 2
    _, per_group, cap, _ = got.shape
    slots = packed.shape[1]
    lanes = per_group * cap
    ffn = inner.shape[1]
    chunk = min(512, width)
    chunks = [pl.ds(c, chunk) for c in range(0, width, chunk)]
    me, dp = lax.axis_index("sp"), lax.axis_index("dp")
    ny = n_sp // GROUPS
    plane, y = me // ny, lax.rem(me, ny)
    member = y * n_dp + dp
    flip = 1 - 2 * lax.rem(plane, 2)
    others = [plane, plane + flip, lax.rem(plane + 2, GROUPS), GROUPS - 1 - plane]

    def at(g, m):
        return (g * ny + m // n_dp, lax.rem(m, n_dp))

    def remote(src, dst, send, recv, device):
        copy = pltpu.make_async_remote_copy(
            src_ref=src,
            dst_ref=dst,
            send_sem=send,
            recv_sem=recv,
            device_id=device,
            device_id_type=MESH,
        )
        copy.start()
        return copy

    def settle(part, sem):
        pltpu.make_async_copy(part, part, sem).wait()

    qkv_loads = [
        pltpu.make_async_copy(queries, q_own, i_sem.at[0]),
        pltpu.make_async_copy(keys_in, k_own, i_sem.at[1]),
        pltpu.make_async_copy(values_in, v_own, i_sem.at[2]),
    ]
    small_loads = [
        pltpu.make_async_copy(src, dst, n_sem.at[i])
        for i, (src, dst) in enumerate(
            (
                (key_shift_hbm, key_shift),
                (head_shift_hbm, head_shift),
                (route_hbm, route),
                (route_weight_hbm, route_weight),
                (mix_gain_hbm, mix_gain),
                (post_gain_hbm, post_gain),
            )
        )
    ]
    for load in qkv_loads + small_loads:
        load.start()
    barrier = pltpu.get_barrier_semaphore()
    for d in range(1, n_sp):
        pl.semaphore_signal(
            barrier, inc=1, device_id=(lax.rem(me + d, n_sp), dp), device_id_type=MESH
        )
    for d in range(1, n_dp):
        for row in range(ny):
            pl.semaphore_signal(
                barrier,
                inc=1,
                device_id=(plane * ny + row, lax.rem(dp + d, n_dp)),
                device_id_type=MESH,
            )

    for load in small_loads[:2]:
        load.wait()

    n_heads = key_shift.shape[0]
    same = lax.broadcasted_iota(jnp.int32, (n_heads, n_heads), 0) == lax.broadcasted_iota(
        jnp.int32, (n_heads, n_heads), 1
    )
    head_column = jnp.sum(jnp.where(same, head_shift[...], 0.0), axis=1, keepdims=True)
    turned = (key_shift[...].astype(F32) + head_column) * LOG2E
    for p in range(n_sp):
        shift_out[p, :heads, :] = turned[p * heads : (p + 1) * heads]
    shift_in[me] = shift_out[me]

    for load in qkv_loads:
        load.wait()
    weight_loads = [
        pltpu.make_async_copy(stream_hbm, stream, w_sem.at[0]),
        pltpu.make_async_copy(out_hbm, out_w, w_sem.at[1]),
        pltpu.make_async_copy(gate_hbm, gate_w, w_sem.at[2]),
        pltpu.make_async_copy(up_hbm, up_w, w_sem.at[3]),
        pltpu.make_async_copy(down_hbm, down_w, w_sem.at[4]),
    ]
    for load in weight_loads:
        load.start()

    def pack_head(h):
        for p in range(n_sp):
            g = p * heads + h
            cols = slice(g * HD, (g + 1) * HD)
            outbox[h, p, :tokens, :] = jnp.concatenate([q_own[:, cols], k_own[:, cols]], axis=1)
            outbox[h, p, tokens:, :] = jnp.concatenate(
                [v_own[:half, cols], v_own[half:, cols]], axis=1
            )
        inbox[h, me] = outbox[h, me]

    order = sorted(range(1, n_sp), key=lambda d: abs(2 * d - n_sp))

    def send_head(h):
        for d in order:
            peer = lax.rem(me + d, n_sp)
            remote(
                outbox.at[h, peer], inbox.at[h, me], q_send.at[h], q_recv.at[h], (peer, dp)
            )

    pack_head(0)
    pl.semaphore_wait(barrier, n_sp - 1 + (n_dp - 1) * ny)
    for d in order:
        peer = lax.rem(me + d, n_sp)
        remote(shift_out.at[peer], shift_in.at[me], s_send.at[0], s_recv.at[0], (peer, dp))
    send_head(0)
    for h in range(1, heads):
        pack_head(h)

    for load in small_loads[2:]:
        load.wait()

    row = lax.broadcasted_iota(jnp.int32, (tokens, tokens), 0)
    col = lax.broadcasted_iota(jnp.int32, (tokens, tokens), 1)
    earlier = ones_where(row > col)
    n_expert = n_sp * n_dp
    wide = max(tokens, n_expert)
    expert = lax.broadcasted_iota(jnp.int32, (tokens, wide), 1).astype(F32)

    def column(values):
        return jnp.sum(jnp.where(row == col, values, 0.0), axis=1, keepdims=True)

    first, second = (column(route[k : k + 1, :].astype(F32)) for k in range(2))
    hit0, hit1 = first == expert, second == expert
    count0 = jnp.dot(earlier, ones_where(hit0), preferred_element_type=F32)
    count1 = jnp.dot(earlier, ones_where(hit1), preferred_element_type=F32) + jnp.dot(
        jnp.ones((tokens, tokens), BF16), ones_where(hit0), preferred_element_type=F32
    )
    rank0 = jnp.sum(jnp.where(hit0, count0, 0.0), axis=1, keepdims=True)
    rank1 = jnp.sum(jnp.where(hit1, count1, 0.0), axis=1, keepdims=True)
    group = jnp.zeros((tokens, 1), F32)
    for g in range(1, GROUPS):
        group = group + jnp.where(first >= float(g * per_group), 1.0, 0.0)
    lane = col.astype(F32)
    in_group = lane == group
    group_count = jnp.dot(earlier, ones_where(in_group), preferred_element_type=F32)
    group_rank = jnp.sum(jnp.where(in_group, group_count, 0.0), axis=1, keepdims=True)
    base = group * per_group
    facts = [
        (first - base) * cap + rank0 + 1.0,
        (second - base) * cap + rank1 + 1.0,
        column(route_weight[0:1, :]),
        column(route_weight[1:2, :]),
    ]
    slot = group * slots + group_rank
    by_lane = jnp.broadcast_to(slot, (tokens, tokens)).T
    slot_row = lax.broadcasted_iota(jnp.int32, (slots, tokens), 0).astype(F32)
    token_hot[...] = ones_where(
        slot == lax.broadcasted_iota(jnp.int32, (tokens, GROUPS * slots), 1).astype(F32)
    )
    for g in range(GROUPS):
        slot_hot[g] = ones_where(by_lane[:slots] - float(g * slots) == slot_row)
        hot = (slot - float(g * slots) == lane) & (col < slots)
        rows = [jnp.sum(jnp.where(hot, f, 0.0), axis=0, keepdims=True) for f in facts]
        rows = [rows[0] - 1.0, rows[1] - 1.0, rows[2], rows[3]]
        meta[g] = jnp.concatenate(rows + [jnp.zeros((4, tokens), F32)], axis=0)
    tables[plane] = meta[plane]

    wide_source = lax.broadcasted_iota(jnp.int32, (2 * tokens, 2 * tokens), 0)
    wide_col = lax.broadcasted_iota(jnp.int32, (2 * tokens, 2 * tokens), 1)
    source = jnp.where(wide_source >= tokens, wide_source - tokens, wide_source)
    summer = jnp.where((wide_col >= tokens) | (source >= wide_col), -1.0, 0.0).astype(BF16)
    pair = 2 if n_sp % 2 == 0 else 1
    span = pair * tokens
    tile_row = lax.broadcasted_iota(jnp.int32, (span, tokens), 0)
    tile_col = lax.broadcasted_iota(jnp.int32, (span, tokens), 1)
    scale = LOG2E / math.sqrt(HD)

    def attend(h, i):
        q = q_all[h, i * span : (i + 1) * span]
        carry = jnp.zeros((span, tokens), F32)
        total = jnp.zeros((span, HD), F32)
        for j in range(i, -1, -1):
            k = k_all[h, j * span : (j + 1) * span]
            z_pair = lax.dot_general(q, k, (((1,), (1,)), ((), ())), preferred_element_type=F32)
            parts = [None] * pair
            for b in range(pair - 1, -1, -1):
                z = z_pair[:, b * tokens : (b + 1) * tokens] * scale
                z = z + shift_in[j * pair + b, h : h + 1, :]
                soft = jnp.maximum(z, jnp.log2(1.0 + jnp.exp2(jnp.minimum(z, 100.0))))
                if i == j:
                    causal = tile_col + b * tokens < tile_row
                    soft = jnp.where(causal, soft, 0.0)
                high = soft.astype(BF16)
                low = (soft - high.astype(F32)).astype(BF16)
                sums = jnp.dot(
                    jnp.concatenate([high, low], axis=1), summer, preferred_element_type=F32
                )
                weight = jnp.exp2(z + (sums[:, :tokens] + carry))
                if i == j:
                    weight = jnp.where(causal, weight, 0.0)
                carry = carry + sums[:, tokens:]
                parts[b] = weight.astype(BF16)
            total = total + jnp.dot(
                jnp.concatenate(parts, axis=1) if pair > 1 else parts[0],
                v_all[h, j * span : (j + 1) * span],
                preferred_element_type=F32,
            )
        for b in range(pair):
            t = i * pair + b
            block = total[b * tokens : (b + 1) * tokens]
            att_out[h, t] = jnp.concatenate([block[:half], block[half:]], axis=1).astype(BF16)
    def return_head(h, i):
        for b in range(pair):
            t = i * pair + b

            @pl.when(me != t)
            def _(t=t):
                remote(
                    att_out.at[h, t], att_in.at[h, me], a_send.at[h], a_recv.at[h], (t, dp)
                )

            @pl.when(me == t)
            def _(t=t):
                att_in[h, t] = att_out[h, t]

    settle(shift_in.at[pl.ds(0, n_sp - 1)], s_recv.at[0])
    for h in range(heads):
        settle(outbox.at[h, pl.ds(0, n_sp - 1)], q_send.at[h])
        if h + 1 < heads:
            send_head(h + 1)
        settle(inbox.at[h, pl.ds(0, n_sp - 1)], q_recv.at[h])
        if h:
            for i in range(n_sp // pair - 1, -1, -1):
                return_head(h - 1, i)
        for j in range(n_sp):
            here = slice(j * tokens, (j + 1) * tokens)
            q_all[h, here] = inbox[h, j, :tokens, :HD]
            k_all[h, here] = inbox[h, j, :tokens, HD:]
            v_all[h, j * tokens : j * tokens + half] = inbox[h, j, tokens:, :HD]
            v_all[h, j * tokens + half : (j + 1) * tokens] = inbox[h, j, tokens:, HD:]
        for i in range(n_sp // pair - 1, -1, -1):
            attend(h, i)
            if h + 1 == heads:
                return_head(h, i)

    for h in range(heads):
        settle(att_in.at[h, pl.ds(0, n_sp - 1)], a_recv.at[h])
        for p in range(n_sp):
            g = p * heads + h
            block = att_in[h, p]
            att[:half, g * HD : (g + 1) * HD] = block[:, :HD]
            att[half:, g * HD : (g + 1) * HD] = block[:, HD:]
    wide_att = att[...].astype(F32)
    ratio = lax.rsqrt(jnp.mean(wide_att * wide_att, axis=1, keepdims=True) + norm_eps)
    normed = (wide_att * ratio * mix_gain[...]).astype(BF16)
    weight_loads[0].wait()
    weight_loads[1].wait()
    square = jnp.zeros((tokens, 1), F32)
    for cols in chunks:
        block = stream[:, cols].astype(F32) + jnp.dot(
            normed, out_w[:, cols], preferred_element_type=F32
        )
        summed[:, cols] = block
        square = square + jnp.sum(block * block, axis=1, keepdims=True)
    ratio = lax.rsqrt(square / width + norm_eps)
    for cols in chunks:
        hidden[:, cols] = (summed[:, cols] * ratio * post_gain[:, cols]).astype(BF16)

    def put_rows(ref, source, cols, rows):
        if cap % 16 == 0:
            ref[source, :, :, cols] = rows.astype(BF16).reshape(per_group, cap, chunk)
        else:
            for m in range(per_group):
                ref[source, m, :, cols] = rows[m * cap : (m + 1) * cap].astype(BF16)

    def take_rows(ref, source, cols):
        if cap % 16 == 0:
            rows = ref[source, :, :, cols]
            return rows.reshape(lanes, rows.shape[-1])
        return jnp.concatenate(
            [ref[source, m, :, cols].astype(F32) for m in range(per_group)], axis=0
        ).astype(BF16)

    z_copies = {}

    def send_plane(k, c):
        q = others[k]
        packed[q, :, chunks[c]] = jnp.dot(
            slot_hot[q], hidden[:, chunks[c]], preferred_element_type=F32
        ).astype(BF16)
        z_copies[k, c] = remote(
            packed.at[q, :, chunks[c]],
            landed.at[plane, :, chunks[c]],
            z_send.at[k, c],
            z_recv.at[k, c],
            at(q, member),
        )

    pieces = range(len(chunks))
    for k in range(1, GROUPS):
        z_copies[k, -1] = remote(
            meta.at[others[k]],
            tables.at[plane],
            t_send.at[k],
            t_recv.at[k],
            at(others[k], member),
        )
    for c in pieces:
        send_plane(3, c)
        send_plane(1, c)
    for cols in chunks:
        landed[plane, :, cols] = jnp.dot(
            slot_hot[plane], hidden[:, cols], preferred_element_type=F32
        ).astype(BF16)

    def fan_out(source, src, dst, cols, send, recv):
        for e in range(1, per_group):
            other = lax.rem(member + e, per_group)
            remote(
                src.at[source, other, :, cols],
                dst.at[source, member, :, cols],
                send,
                recv,
                at(plane, other),
            )
        dst[source, member, :, cols] = src[source, member, :, cols]

    def group_wait(source, ref, cols, sem):
        settle(ref.at[source, pl.ds(0, per_group - 1), :, cols], sem)

    hots = {}

    def deliver(k, c):
        source = others[k]
        if k not in hots:
            if k:
                z_copies[k, -1].wait_recv()
            info = tables[source]
            hots[k] = ones_where(one_hot_rows(info, 0) | one_hot_rows(info, 1))[:, :slots]
        if k:
            z_copies[k, c].wait_recv()
        rows = jnp.dot(hots[k], landed[source, :, chunks[c]], preferred_element_type=F32)
        put_rows(stage, source, chunks[c], rows)
        fan_out(source, stage, got, chunks[c], p_send.at[k, c], p_recv.at[k, c])

    loaded = []

    def experts(k, send):
        source = others[k]
        for c, cols in enumerate(chunks):
            group_wait(source, got, cols, p_recv.at[k, c])
        if not loaded:
            loaded.append(True)
            for load in weight_loads[2:]:
                load.wait()
        rows = take_rows(got, source, slice(None))
        part = min(256, ffn)
        for n in range(0, ffn, part):
            gate = jnp.dot(rows, gate_w[:, n : n + part], preferred_element_type=F32)
            upper = jnp.dot(rows, up_w[:, n : n + part], preferred_element_type=F32)
            inner[:, n : n + part] = (gate / (1.0 + jnp.exp(-gate)) * upper).astype(BF16)
        for c, cols in enumerate(chunks):
            out = jnp.dot(inner[...], down_w[:, cols], preferred_element_type=F32)
            put_rows(reply, source, cols, out)
            if send:
                answer(k, c)

    def answer(k, c):
        fan_out(others[k], reply, back, chunks[c], r_send.at[k, c], r_recv.at[k, c])

    y_copies = {}

    spreads = {}

    def combine(k, c):
        source = others[k]
        cols = chunks[c]
        if k not in spreads:
            info = tables[source]
            spread = jnp.where(one_hot_rows(info, 0), info[2:3, :], 0.0) + jnp.where(
                one_hot_rows(info, 1), info[3:4, :], 0.0
            )
            spread = spread.T[:slots]
            high = spread.astype(BF16)
            spreads[k] = high, (spread - high.astype(F32)).astype(BF16)
        high, low = spreads[k]
        group_wait(source, back, cols, r_recv.at[k, c])
        rows = take_rows(back, source, cols)
        total = jnp.dot(high, rows, preferred_element_type=F32) + jnp.dot(
            low, rows, preferred_element_type=F32
        )
        if k:
            partial[source, :, cols] = total.astype(BF16)
            y_copies[k, c] = remote(
                partial.at[source, :, cols],
                returned.at[plane, :, cols],
                y_send.at[k, c],
                y_recv.at[k, c],
                at(source, member),
            )
        else:
            returned[source, :, cols] = total.astype(BF16)

    for c in pieces:
        deliver(0, c)
    for c in pieces:
        deliver(1, c)
        deliver(3, c)
        send_plane(2, c)
    experts(0, False)
    experts(3, False)
    experts(1, False)
    for c in pieces:
        deliver(2, c)
    for c in pieces:
        answer(3, c)
    experts(2, False)
    for c in pieces:
        combine(3, c)
        answer(2, c)
    for c in pieces:
        combine(2, c)
        answer(1, c)
    for c in pieces:
        combine(1, c)
        answer(0, c)
    for c in pieces:
        combine(0, c)

    for c, cols in enumerate(chunks):
        for k in range(1, GROUPS):
            y_copies[k, c].wait_recv()
        rows = returned[:, :, cols].reshape(GROUPS * slots, chunk)
        total = jnp.dot(token_hot[...], rows, preferred_element_type=F32)
        result[:, cols] = (hidden[:, cols].astype(F32) + total).astype(BF16)

    settle(shift_out.at[pl.ds(0, n_sp - 1)], s_send.at[0])
    for h in range(heads):
        settle(att_out.at[h, pl.ds(0, n_sp - 1)], a_send.at[h])
    for k in range(GROUPS):
        for c, cols in enumerate(chunks):
            if k:
                z_copies[k, c].wait_send()
                y_copies[k, c].wait_send()
            group_wait(others[k], stage, cols, p_send.at[k, c])
            group_wait(others[k], reply, cols, r_send.at[k, c])
        if k:
            z_copies[k, -1].wait_send()


def on_device(
    n_sp,
    n_dp,
    stream,
    queries,
    keys_in,
    values_in,
    key_shift,
    head_shift,
    mix_gain,
    out_weight,
    post_gain,
    route,
    route_weight,
    w_gate,
    w_up,
    w_down,
):
    tokens, width = stream.shape[1:]
    n_heads = key_shift.shape[2]
    heads = n_heads // n_sp
    mixer = queries.shape[2]
    ffn = w_gate.shape[2]
    per_group = n_sp * n_dp // GROUPS
    cap = tokens // per_group
    slots = tokens // 2
    chunks = width // min(512, width)
    dma = pltpu.SemaphoreType.DMA
    own = pltpu.VMEM((tokens, mixer), BF16)
    box = pltpu.VMEM((heads, n_sp, tokens + tokens // 2, 2 * HD), BF16)
    shifts = pltpu.VMEM((n_sp, 8, tokens), F32)
    line = pltpu.VMEM((heads, n_sp * tokens, HD), BF16)
    att_box = pltpu.VMEM((heads, n_sp, tokens // 2, 2 * HD), BF16)
    table = pltpu.VMEM((GROUPS, 8, tokens), F32)
    wide = pltpu.VMEM((GROUPS, per_group, cap, width), BF16)
    narrow = pltpu.VMEM((GROUPS, slots, width), BF16)
    here = pl.BlockSpec(memory_space=pltpu.VMEM)
    there = pl.BlockSpec(memory_space=pl.ANY)
    out = pl.pallas_call(
        functools.partial(layer_kernel, n_sp, n_dp),
        out_shape=pltpu.VMEM((tokens, width), BF16),
        in_specs=[there] * 14,
        out_specs=here,
        scratch_shapes=[
            pltpu.VMEM((n_heads, tokens), BF16),
            pltpu.VMEM((1, n_heads), F32),
            pltpu.VMEM((1, mixer), F32),
            pltpu.VMEM((1, width), F32),
            pltpu.VMEM((2, tokens), jnp.int32),
            pltpu.VMEM((2, tokens), F32),
            own,
            own,
            own,
            box,
            box,
            shifts,
            shifts,
            line,
            line,
            line,
            att_box,
            att_box,
            own,
            pltpu.VMEM((tokens, width), BF16),
            pltpu.VMEM((tokens, width), F32),
            pltpu.VMEM((tokens, width), BF16),
            table,
            pltpu.VMEM((GROUPS, slots, tokens), BF16),
            pltpu.VMEM((tokens, GROUPS * slots), BF16),
            narrow,
            narrow,
            table,
            wide,
            wide,
            pltpu.VMEM((per_group * cap, ffn), BF16),
            wide,
            wide,
            narrow,
            narrow,
            pltpu.VMEM((mixer, width), BF16),
            pltpu.VMEM((width, ffn), BF16),
            pltpu.VMEM((width, ffn), BF16),
            pltpu.VMEM((ffn, width), BF16),
            dma((3,)),
            dma((6,)),
            dma((5,)),
            dma((1,)),
            dma((1,)),
            dma((heads,)),
            dma((heads,)),
            dma((heads,)),
            dma((heads,)),
            dma((GROUPS,)),
            dma((GROUPS,)),
        ]
        + [dma((GROUPS, chunks))] * 8,
        compiler_params=pltpu.CompilerParams(
            collective_id=0, has_side_effects=True, vmem_limit_bytes=VLIM
        ),
        name="layer",
    )(
        queries[0],
        keys_in[0],
        values_in[0],
        key_shift[0].T,
        head_shift[None],
        mix_gain[None],
        out_weight,
        post_gain[None],
        stream[0],
        route[0].T,
        route_weight[0].T,
        w_gate[0],
        w_up[0],
        w_down[0],
    )
    return out[None]


def solution(mesh):
    return jax.shard_map(
        functools.partial(on_device, mesh.shape["sp"], mesh.shape["dp"]),
        mesh=mesh,
        in_specs=(
            P("dp", "sp", None),
            P("dp", "sp", None),
            P("dp", "sp", None),
            P("dp", "sp", None),
            P("dp", "sp", None),
            P(),
            P(),
            P(),
            P(),
            P("dp", "sp", None),
            P("dp", "sp", None),
            P(("sp", "dp"), None, None),
            P(("sp", "dp"), None, None),
            P(("sp", "dp"), None, None),
        ),
        out_specs=P("dp", "sp", None),
        check_vma=False,
    )
```
